1024 devices in a mesh: ep: 32 (over z, core), tp: 32 (over y, x).
Axes of the slice: x: 4, y: 8, z: 16, core: 2. Of those that a mesh axis runs over, the one named last changes fastest.
Arguments:
- tokens: bfloat16 [256, 2048], P('ep'), may hold values from -6 to 6
- attn_gain: float32 [2048], replicated, may hold values from 0.1 to 1.9
- query_weight: bfloat16 [2048, 4096], P('ep', 'tp'), may hold values from -0.125 to 0.125
- key_weight: bfloat16 [2048, 4096], P('ep', 'tp'), may hold values from -0.125 to 0.125
- value_weight: bfloat16 [2048, 4096], P('ep', 'tp'), may hold values from -0.125 to 0.125
- query_gain: float32 [128], replicated, may hold values from 0.1 to 1.9
- stick_bias: float32 [32], P('tp'), may hold values from -7 to -2.5
- key_cache: bfloat16 [256, 32, 512, 128], P('ep', 'tp'), may hold values from -6 to 6
- value_cache: bfloat16 [256, 32, 512, 128], P('ep', 'tp'), may hold values from -6 to 6
- lengths: int32 [256], P('ep'), may hold values from 64 to 512, as said below
- out_weight: bfloat16 [4096, 2048], P('tp'), may hold values from -0.375 to 0.375
- mix_gain: float32 [2048], replicated, may hold values from 0.1 to 1.9
- route_ids: int32 [256, 2], P('ep'), may hold values from 0 to 31, all different within a row; in each aligned block of 8 rows (0 to 7, 8 to 15, ...) at most 2 rows name the same one
- route_weights: float32 [256, 2], P('ep'), may hold values from 0.2 to 1
- expert_gate: bfloat16 [32, 2048, 2560], P('ep', None, 'tp'), may hold values from -0.125 to 0.125
- expert_up: bfloat16 [32, 2048, 2560], P('ep', None, 'tp'), may hold values from -0.125 to 0.125
- expert_down: bfloat16 [32, 2560, 2048], P('ep', 'tp'), may hold values from -0.21875 to 0.21875
- side_gate: bfloat16 [2048, 1024], P(None, 'tp'), may hold values from -0.125 to 0.125
- side_up: bfloat16 [2048, 1024], P(None, 'tp'), may hold values from -0.125 to 0.125
- side_down: bfloat16 [1024, 2048], P('tp'), may hold values from -0.375 to 0.375
- branch_gate: float32 [2048], replicated, may hold values from -0.125 to 0.125
Outputs:
- mixed: bfloat16 [256, 2048], P('ep', 'tp')
- new_keys: bfloat16 [256, 4096], P('ep', 'tp')
- new_values: bfloat16 [256, 4096], P('ep', 'tp')
The draws below stay inside these ranges and needn't reach their ends.
Inputs may be any that keep to these rules, and one draw needn't show every extreme that they name: `lengths`: at least an eighth of 512; the first sequence has 512. `route_ids`: each token names 2 different experts. In the rows of one device no expert is named by more than 2 rows, a bound that some block reaches of some device.
All inputs are finite; a program needn't handle non-finite values.
Results may differ from the reference program's by a relative error of at most 0.018.
Values may be sent and summed in bfloat16 or wider, within the bound.
A program may use at most 32 MiB of HBM per device.

```python
import math
import jax
import jax.numpy as jnp
import numpy as np
from jax import lax

D = 2048
H = 32
DH = 128
FF_E = 2560
SH = 1024
TOP = 2
SEQS = 8
L = 512
BATCH = 256
E = 32
CAP = 2
N_EP = 32


def draw_lengths(key, part):
    drawn = jax.random.randint(key, (BATCH,), L // 8, L + 1, dtype=jnp.int32)
    return drawn.at[0].set(L)


def raised(result, key, source, target, shards_of, factor):
    owner, partner = [(jnp.arange(result.shape[axis_at]) // (result.shape[axis_at] // shards_of)).reshape([-1 if axis == axis_at else 1 for axis in range(result.ndim)]) for axis_at in (source, target)]
    chosen = jax.random.permutation(key, shards_of)[partner]
    strong = (owner == chosen) | (owner == (partner + shards_of // 2) % shards_of)
    return jnp.where(strong, factor * result, result)


def level_of(key, dims, pieces, low, high):
    gain = 1.0
    for axis_at, parts in pieces:
        steps = jax.random.uniform(jax.random.fold_in(jax.random.fold_in(key, 6), axis_at), (parts,), jnp.float32, low / len(pieces), high / len(pieces))
        gain = gain * jnp.repeat(jnp.exp(steps), dims[axis_at] // parts).reshape((-1,) + (1,) * (len(dims) - 1 - axis_at))
    return gain


def routed_block(own_key, own, number, rows, amount, top, bound, lean):
    ranking = jax.random.permutation(own_key, amount)
    crowded, ordinary = portions_of(amount, rows * top, bound, lean, True), portions_of(amount, rows * top, bound, lean, False)
    places = jnp.arange(amount)

    def named(sizes, rotation):
        used = int((sizes > 0).sum())
        fixed = max(1, used // 4)
        moved = fixed + (places - fixed + rotation * (used - fixed)) % max(1, amount - fixed)
        return jnp.zeros((amount,), jnp.int32).at[ranking[jnp.where(places < fixed, places, moved)]].set(jnp.asarray(sizes, jnp.int32))

    sizes = jnp.where(number % 4 == 0, named(crowded, number // 4), named(ordinary, number - number // 4 - 1))
    mixed = jax.random.permutation(jax.random.fold_in(own, 3), amount)
    source_of, receiver = mixed[0:amount // 2 * 2:2], mixed[1:amount // 2 * 2:2]
    margin = jnp.minimum(sizes[source_of] - 1, bound - sizes[receiver]) // 2
    margin = jnp.where((source_of == ranking[0]) | (receiver == ranking[0]) | (sizes[receiver] == 0), 0, jnp.maximum(margin, 0))
    moved = jax.random.randint(jax.random.fold_in(own, 4), (amount // 2,), 0, 1 << 20) % (margin + 1)
    sizes = sizes.at[source_of].add(-moved).at[receiver].add(moved)
    items = jnp.searchsorted(jnp.cumsum(sizes), jnp.arange(rows * top), side="right").astype(jnp.int32)
    grid = items.reshape(top, rows).T
    grid = grid[jax.random.permutation(jax.random.fold_in(own, 1), rows)]
    rotation = jax.random.randint(jax.random.fold_in(own, 2), (rows, 1), 0, top)
    return jnp.take_along_axis(grid, (jnp.arange(top)[None, :] + rotation) % top, axis=1)


def portions_of(number_of, total, limit, slope, full):
    weights = [(1 << 20) // math.isqrt(standing ** slope) + 1 for standing in range(1, number_of + 1)]
    largest = limit if full else min(limit, max(-(-total // number_of), total * weights[0] // sum(weights)))
    least = 1 if total - largest >= number_of - 1 else 0
    counts, rest = [largest] + [least] * (number_of - 1), total - largest - least * (number_of - 1)
    while rest > 0:
        candidates = [i for i in range(1, number_of) if counts[i] < largest] or [i for i in range(1, number_of) if counts[i] < limit]
        pool, remaining = sum([weights[i] for i in candidates]), rest
        for i in candidates:
            addition = min(limit - counts[i], max(1, remaining * weights[i] // pool), rest)
            counts[i] = counts[i] + addition
            rest = rest - addition
    return np.array(counts)


def gaussian(key, extent, deviation, reach, split=(), kind=jnp.bfloat16):
    level = level_of(key, extent, split, -0.22, 0.18) if split else 1.0
    entries = jax.random.normal(key, extent, jnp.float32) * deviation * level
    return jnp.minimum(jnp.maximum(entries, -reach), reach).astype(kind)


def gaussian_with(own_key, shape, deviation, limit, split, heavy, held_as=jnp.bfloat16):
    entries = deviation * jax.random.normal(own_key, shape, jnp.float32)
    if split:
        entries = entries * level_of(own_key, shape, split, -0.22, 0.18)
    return jnp.clip(raised(entries, jax.random.fold_in(own_key, 3), *heavy), -limit, limit).astype(held_as)


def setup_inputs(seed: int = 0) -> dict:
    keys = jax.random.split(jax.random.key(seed), 22)
    tokens = gaussian(keys[0], (BATCH, D), 1.0, 6.0, ((0, 32),))
    attn_gain = jnp.clip(1.0 + 0.18 * jax.random.normal(keys[1], (D,), jnp.float32), 0.1, 1.9)
    query_weight = gaussian(keys[2], (D, H * DH), D ** -0.5, 0.125, ((0, 32), (1, 32)))
    key_weight = gaussian(keys[3], (D, H * DH), D ** -0.5, 0.125, ((0, 32), (1, 32)))
    value_weight = gaussian(keys[4], (D, H * DH), D ** -0.5, 0.125, ((0, 32), (1, 32)))
    query_gain = jnp.clip(1.0 + 0.18 * jax.random.normal(keys[5], (DH,), jnp.float32), 0.1, 1.9)
    stick_bias = jnp.clip(-7.0 + 4.5 * jax.random.uniform(keys[6], (H,), jnp.float32) ** level_of(keys[6], (H,), ((0, 32),), -0.2, 0.2), -7.0, -2.5)
    key_cache = gaussian(keys[7], (BATCH, H, L, DH), 1.0, 6.0, ((0, 32), (1, 32)))
    value_cache = gaussian(keys[8], (BATCH, H, L, DH), 1.0, 6.0, ((0, 32), (1, 32)))
    lengths = draw_lengths(jax.random.fold_in(keys[21], 71), 0)
    out_weight = gaussian(keys[10], (H * DH, D), (H * DH // 16) ** -0.5, 0.375, ((0, 32),))
    mix_gain = jnp.clip(1.0 + 0.18 * jax.random.normal(keys[11], (D,), jnp.float32), 0.1, 1.9)
    route_ids_keys = jax.random.split(jax.random.fold_in(keys[12], 1), BATCH // SEQS)
    route_ids_turns = jax.random.permutation(jax.random.fold_in(keys[12], 3), BATCH // SEQS)
    route_ids = jax.vmap(lambda own, number: routed_block(jax.random.fold_in(keys[12], 2), own, number, SEQS, E, TOP, CAP, 2))(route_ids_keys, route_ids_turns).reshape((BATCH, TOP))
    route_weights = jnp.clip(0.2 + 0.8 * jax.random.uniform(keys[13], (BATCH, TOP), jnp.float32) ** level_of(keys[13], (BATCH, TOP), ((0, 32),), -0.2, 0.2), 0.2, 1.0)
    expert_gate = gaussian(keys[14], (E, D, FF_E), D ** -0.5, 0.125, ((0, 32), (2, 32)))
    expert_up = gaussian(keys[15], (E, D, FF_E), D ** -0.5, 0.125, ((0, 32), (2, 32)))
    expert_down = gaussian_with(keys[16], (E, FF_E, D), FF_E ** -0.5, 0.21875, ((0, 32), (1, 32)), (1, 2, 32, 2.75))
    side_gate = gaussian(keys[17], (D, SH), D ** -0.5, 0.125, ((1, 32),))
    side_up = gaussian(keys[18], (D, SH), D ** -0.5, 0.125, ((1, 32),))
    side_down = gaussian_with(keys[19], (SH, D), SH ** -0.5, 0.375, ((0, 32),), (0, 1, 32, 2.75))
    branch_gate = gaussian(keys[20], (D,), D ** -0.5, 0.125, (), jnp.float32)
    return dict(tokens=tokens, attn_gain=attn_gain, query_weight=query_weight, key_weight=key_weight, value_weight=value_weight, query_gain=query_gain, stick_bias=stick_bias, key_cache=key_cache, value_cache=value_cache, lengths=lengths, out_weight=out_weight, mix_gain=mix_gain, route_ids=route_ids, route_weights=route_weights, expert_gate=expert_gate, expert_up=expert_up, expert_down=expert_down, side_gate=side_gate, side_up=side_up, side_down=side_down, branch_gate=branch_gate)


epsilon = 1e-06

def rms_scale(values, scale_gain):
    mean_square = lax.optimization_barrier(jnp.mean(values * values, axis=-1, keepdims=True))
    return values * lax.rsqrt(mean_square + epsilon) * scale_gain

def expert_apply(bundle):
    slot_rows, gate_w, up_w, down_w = bundle
    gate_pre = jnp.dot(slot_rows, gate_w, preferred_element_type=jnp.float32)
    up_pre = jnp.dot(slot_rows, up_w, preferred_element_type=jnp.float32)
    hidden = (jax.nn.silu(gate_pre) * up_pre).astype(jnp.bfloat16)
    return jnp.dot(hidden, down_w, preferred_element_type=jnp.float32).astype(jnp.bfloat16)

def reference(tokens, attn_gain, query_weight, key_weight, value_weight, query_gain, stick_bias, key_cache, value_cache, lengths, out_weight, mix_gain, route_ids, route_weights, expert_gate, expert_up, expert_down, side_gate, side_up, side_down, branch_gate):
    stream = tokens.astype(jnp.float32)
    normed = rms_scale(stream, attn_gain).astype(jnp.bfloat16)
    query_rows = jnp.dot(normed, query_weight, preferred_element_type=jnp.float32).astype(jnp.bfloat16)
    fresh_keys = jnp.dot(normed, key_weight, preferred_element_type=jnp.float32).astype(jnp.bfloat16)
    new_values = jnp.dot(normed, value_weight, preferred_element_type=jnp.float32).astype(jnp.bfloat16)
    batch_count = tokens.shape[0]
    new_keys = rms_scale(fresh_keys.astype(jnp.float32).reshape(batch_count, H, DH), 1.0)
    new_keys = new_keys.astype(jnp.bfloat16).reshape(batch_count, H * DH)
    query_heads = rms_scale(query_rows.astype(jnp.float32).reshape(batch_count, H, DH), query_gain)
    query_heads = query_heads.astype(jnp.bfloat16)

    def attend_one(bundle):
        query_row, key_rows, value_rows, length = bundle
        scores = jnp.einsum('hd,hld->hl', query_row.astype(jnp.float32), key_rows.astype(jnp.float32))
        scores = scores * DH ** (-0.5) + stick_bias[:, None]
        positions = jnp.arange(L, dtype=jnp.int32)
        visible = positions[None, :] < length
        log_rest = jnp.where(visible, jax.nn.log_sigmoid(-scores), 0.0)
        log_between = lax.cumsum(log_rest, axis=1, reverse=True) - log_rest
        stick = jnp.where(visible, jnp.exp(jax.nn.log_sigmoid(scores) + log_between), 0.0).astype(jnp.bfloat16)
        attended = jnp.einsum('hl,hld->hd', stick.astype(jnp.float32), value_rows.astype(jnp.float32))
        return attended.astype(jnp.bfloat16).reshape(H * DH)
    attended = lax.map(attend_one, (query_heads, key_cache, value_cache, lengths))
    attn_proj = jnp.dot(attended, out_weight, preferred_element_type=jnp.float32)
    middle = (stream + attn_proj).astype(jnp.bfloat16)
    normed_mix = rms_scale(middle.astype(jnp.float32), mix_gain).astype(jnp.bfloat16)
    flat_ids = route_ids.reshape(N_EP, SEQS * TOP)
    onehot = (flat_ids[:, :, None] == jnp.arange(E, dtype=jnp.int32)[None, None, :]).astype(jnp.int32)
    before = jnp.cumsum(onehot, axis=1) - onehot
    slot_index = lax.optimization_barrier(jnp.sum(before * onehot, axis=2))
    sources = jnp.arange(N_EP, dtype=jnp.int32)[:, None]
    target = ((flat_ids * N_EP + sources) * CAP + slot_index).reshape(-1).astype(jnp.int32)
    slot_table = jnp.zeros((E * N_EP * CAP,), jnp.int32).at[target].set(jnp.arange(BATCH * TOP, dtype=jnp.int32))
    slot_rows = normed_mix[slot_table // TOP].reshape(E, N_EP * CAP, D)
    expert_outs = lax.map(expert_apply, (slot_rows, expert_gate, expert_up, expert_down))
    route_out = expert_outs.reshape(E * N_EP * CAP, D)[target].astype(jnp.float32).reshape(BATCH, TOP, D)
    routed = lax.optimization_barrier(jnp.sum(route_weights[:, :, None] * route_out, axis=1))
    side_gate_pre = jnp.dot(normed_mix, side_gate, preferred_element_type=jnp.float32)
    side_up_pre = jnp.dot(normed_mix, side_up, preferred_element_type=jnp.float32)
    side_hidden = (jax.nn.silu(side_gate_pre) * side_up_pre).astype(jnp.bfloat16)
    side_out = jnp.dot(side_hidden, side_down, preferred_element_type=jnp.float32)
    switch = jax.nn.sigmoid(lax.optimization_barrier(jnp.sum(normed_mix.astype(jnp.float32) * branch_gate, axis=1, keepdims=True)))
    mixed = (middle.astype(jnp.float32) + routed + switch * side_out).astype(jnp.bfloat16)
    return (mixed, new_keys, new_values)
```

```python
import functools

import jax
import jax.numpy as jnp
from jax import lax
from jax.experimental import pallas as pl
from jax.experimental.pallas import tpu as pltpu
from jax.sharding import PartitionSpec as P

DH = 128
XN = 4
EPS = 1e-06
F32 = jnp.float32
BF16 = jnp.bfloat16
MESH = pl.DeviceIdType.MESH


def far_first(i, n):
    half = (i + 1) // 2
    return n // 2 + half * (2 * lax.rem(i + 1, 2) - 1)


def log_sigmoids(x):
    t = jnp.log1p(jnp.exp(-jnp.abs(x)))
    return jnp.minimum(x, 0.0) - t, jnp.minimum(-x, 0.0) - t


def kernel(
    ep_n,
    tp_n,
    tokens,
    attn_gain,
    wq,
    wk,
    wv,
    qgain,
    bias,
    kcache,
    vcache,
    lengths,
    oweight,
    mix_gain,
    rids,
    rweights,
    egate,
    eup,
    edown,
    sgate,
    sup,
    sdown,
    bgate,
    mixed_out,
    keys_out,
    values_out,
    tok,
    again,
    mgain,
    qg,
    bg,
    wpad,
    kb,
    vb,
    ow,
    eg,
    eu,
    ed,
    sg,
    su,
    sd,
    tri,
    tiles,
    nsend,
    nrecv,
    qsend,
    qrecv,
    kvsend,
    kvrecv,
    asend,
    arecv,
    mid,
    nmix,
    xo,
    obox,
    ibox,
    xt,
    xg,
    xn,
    ssend,
    srecv,
    esend,
    erecv,
    rsend,
    rrecv,
    ld,
    snd,
    rcv,
):
    me_e = lax.axis_index("ep")
    me_t = lax.axis_index("tp")
    core = lax.rem(me_e, 2)
    yn = tp_n // XN
    my_y = me_t // XN
    my_x = lax.rem(me_t, XN)
    my_k = me_t // 2
    side = lax.rem(me_t, 2)
    kt = tp_n // 2
    seqs, width = tok.shape
    slots = kb.shape[1]

    def ep_peer(i):
        return lax.rem(me_e + far_first(i, ep_n), ep_n)

    def tp_peer(i):
        dy = far_first(i // XN, yn)
        dx = far_first(lax.rem(i, XN), XN)
        return lax.rem(my_y + dy, yn) * XN + lax.rem(my_x + dx, XN)

    barrier = pltpu.get_barrier_semaphore()

    def greet_ep(i, c):
        pl.semaphore_signal(barrier, inc=1, device_id={"ep": ep_peer(i)}, device_id_type=MESH)
        return c

    def greet_tp(i, c):
        pl.semaphore_signal(barrier, inc=1, device_id={"tp": tp_peer(i)}, device_id_type=MESH)
        return c

    lax.fori_loop(0, ep_n - 1, greet_ep, 0)
    lax.fori_loop(0, tp_n - 1, greet_tp, 0)

    rows_w = wq.shape[0]
    at_w = pl.ds(pl.multiple_of(core * rows_w, rows_w), rows_w)
    loads = [
        (tokens, tok),
        (attn_gain, again),
        (wq, wpad.at[at_w, pl.ds(0, DH)]),
        (wk, wpad.at[at_w, pl.ds(DH, DH)]),
        (wv, wpad.at[at_w, pl.ds(2 * DH, DH)]),
        (qgain, qg),
        (kcache.at[:, 0], kb),
        (vcache.at[:, 0], vb),
        (oweight, ow),
        (mix_gain, mgain),
        (bgate, bg),
        (sgate, sg),
        (sup, su),
        (sdown, sd),
        (egate.at[0], eg),
        (eup.at[0], eu),
        (edown.at[0], ed),
    ]
    copies = [pltpu.make_async_copy(a, b, ld.at[i]) for i, (a, b) in enumerate(loads)]
    for c in copies:
        c.start()

    other = pl.ds(pl.multiple_of((1 - core) * rows_w, rows_w), rows_w)
    wpad[other, :] = jnp.zeros((rows_w, 3 * DH), BF16)
    r_i = lax.broadcasted_iota(jnp.int32, (slots, slots), 0)
    c_i = lax.broadcasted_iota(jnp.int32, (slots, slots), 1)
    tri[...] = jnp.where(r_i > c_i, 1.0, 0.0).astype(BF16)

    ids = [rids[b, k] for b in range(seqs) for k in range(2)]
    places = []
    for i in range(2 * seqs):
        n = jnp.int32(0)
        for j in range(i):
            if j // 2 != i // 2:
                n = n + jnp.where(ids[j] == ids[i], 1, 0)
        places.append(n)

    copies[0].wait()
    copies[1].wait()
    stream = tok[...].astype(F32)
    ms = jnp.mean(stream * stream, axis=-1, keepdims=True)
    normed = (stream * lax.rsqrt(ms + EPS) * again[...]).astype(BF16)
    for k in range(kt):
        tiles[k] = stream[:, k * 128 : (k + 1) * 128]
        nsend[k] = normed[:, k * 128 : (k + 1) * 128]
    nrecv[me_e] = nsend[me_e // 2]

    pl.semaphore_wait(barrier, ep_n + tp_n - 2)

    def put_ep(p, src_of, dst):
        def one(i, c):
            f = ep_peer(i)
            pltpu.make_async_remote_copy(
                src_ref=src_of(f),
                dst_ref=dst.at[me_e],
                send_sem=snd.at[p],
                recv_sem=rcv.at[p],
                device_id={"ep": f},
                device_id_type=MESH,
            ).start()
            return c

        lax.fori_loop(0, ep_n - 1, one, 0)

    def put_tp(p, src_of, dst):
        def one(i, c):
            f = tp_peer(i)
            pltpu.make_async_remote_copy(
                src_ref=src_of(f),
                dst_ref=dst.at[me_t],
                send_sem=snd.at[p],
                recv_sem=rcv.at[p],
                device_id={"tp": f},
                device_id_type=MESH,
            ).start()
            return c

        lax.fori_loop(0, tp_n - 1, one, 0)

    def put_tiles(p, buf):
        def one(i, c):
            q = lax.rem(i + 1, 2)
            y = lax.rem(my_y + far_first(i // 2, yn), yn)
            f = y * XN + q * (XN - 1 - my_x) + (1 - q) * my_x
            pltpu.make_async_remote_copy(
                src_ref=buf.at[my_k],
                dst_ref=buf.at[my_k],
                send_sem=snd.at[p],
                recv_sem=rcv.at[p],
                device_id={"tp": f},
                device_id_type=MESH,
            ).start()
            return c

        lax.fori_loop(0, 2 * yn - 1, one, 0)

    def arrived(p, buf, n):
        part = buf.at[pl.ds(0, n)]
        pltpu.make_async_copy(part, part, rcv.at[p]).wait()

    def sent(p, buf, n):
        part = buf.at[pl.ds(0, n)]
        pltpu.make_async_copy(part, part, snd.at[p]).wait()

    put_ep(0, lambda f: nsend.at[f // 2], nrecv)
    for i in (2, 3, 4, 5):
        copies[i].wait()
    arrived(0, nrecv, ep_n - 1)
    picked = nrecv[...].astype(F32).reshape(ep_n * seqs, 128).astype(BF16)
    part = jnp.dot(picked, wpad[:, :DH], preferred_element_type=F32)
    for f in range(ep_n):
        qsend[f] = part[f * seqs : (f + 1) * seqs].astype(BF16)
    put_ep(1, lambda f: qsend.at[f], qrecv)
    qrecv[me_e] = qsend[me_e]
    part = jnp.dot(picked, wpad[:, DH:], preferred_element_type=F32)
    for f in range(ep_n):
        kvsend[f, 0] = part[f * seqs : (f + 1) * seqs, :DH].astype(BF16)
        kvsend[f, 1] = part[f * seqs : (f + 1) * seqs, DH:].astype(BF16)
    put_ep(2, lambda f: kvsend.at[f], kvrecv)
    kvrecv[me_e] = kvsend[me_e]

    row = lax.broadcasted_iota(jnp.int32, (seqs, slots), 0)
    pos = lax.broadcasted_iota(jnp.int32, (seqs, slots), 1)
    lens = jnp.zeros((seqs, slots), jnp.int32)
    for b in range(seqs):
        lens = jnp.where(row == b, lengths[b], lens)
    visible = pos < lens
    copies[6].wait()
    copies[7].wait()
    copies[8].wait()
    arrived(1, qrecv, ep_n - 1)
    q = jnp.sum(qrecv[...].astype(F32), axis=0).astype(BF16).astype(F32)
    ms = jnp.mean(q * q, axis=-1, keepdims=True)
    q = (q * lax.rsqrt(ms + EPS) * qg[...]).astype(BF16)
    scores = jnp.zeros((seqs, slots), F32)
    for b in range(seqs):
        s = lax.dot_general(q, kb[b], (((1,), (1,)), ((), ())), preferred_element_type=F32)
        scores = jnp.where(row == b, s, scores)
    scores = scores * DH ** (-0.5) + bias[0]
    take, rest = log_sigmoids(scores)
    rest = jnp.where(visible, rest, 0.0)
    hi = rest.astype(BF16)
    left = rest - hi.astype(F32)
    lo = left.astype(BF16)
    last = (left - lo.astype(F32)).astype(BF16)
    t = tri[...]
    between = (
        jnp.dot(hi, t, preferred_element_type=F32)
        + jnp.dot(lo, t, preferred_element_type=F32)
        + jnp.dot(last, t, preferred_element_type=F32)
    )
    stick = jnp.where(visible, jnp.exp(take + between), 0.0)
    att = jnp.zeros((seqs, DH), F32)
    for b in range(seqs):
        only = jnp.where(row == b, stick, 0.0).astype(BF16)
        att = att + jnp.dot(only, vb[b], preferred_element_type=F32)
    att = att.astype(BF16)
    proj = jnp.dot(att, ow[...], preferred_element_type=F32)
    for k in range(kt):
        asend[k] = proj[:, k * 128 : (k + 1) * 128].astype(BF16)
    put_tp(3, lambda f: asend.at[f // 2], arecv)
    arecv[me_t] = asend[my_k]

    arrived(2, kvrecv, ep_n - 1)
    fresh = jnp.sum(kvrecv[:, 0].astype(F32), axis=0).astype(BF16).astype(F32)
    ms = jnp.mean(fresh * fresh, axis=-1, keepdims=True)
    keys_out[...] = (fresh * lax.rsqrt(ms + EPS)).astype(BF16)
    values_out[...] = jnp.sum(kvrecv[:, 1].astype(F32), axis=0).astype(BF16)

    arrived(3, arecv, tp_n - 1)
    middle = (tiles[my_k] + jnp.sum(arecv[...].astype(F32), axis=0)).astype(BF16)
    mid[my_k] = middle
    middle = middle.astype(F32)
    slot_row = lax.broadcasted_iota(jnp.int32, (2 * ep_n, 128), 0)
    outbox = jnp.zeros((2 * ep_n, 128), F32)
    for i in range(2 * seqs):
        b = i // 2
        outbox = jnp.where(slot_row == places[i] * ep_n + ids[i], middle[b : b + 1, :], outbox)
    xo[...] = outbox
    for e in range(ep_n):
        obox[e, :, 0:128] = xo[e : e + 1, :]
        obox[e, :, 128:256] = xo[ep_n + e : ep_n + e + 1, :]
    put_ep(4, lambda f: obox.at[f], ibox)
    put_tiles(5, mid)
    ibox[me_e] = obox[me_e]

    for i in (9, 10, 11, 12, 13):
        copies[i].wait()
    arrived(5, mid, 2 * yn - 1)
    ss = jnp.zeros((seqs, 128), F32)
    for k in range(kt):
        m = mid[k].astype(F32)
        ss = ss + m * m
    scale = lax.rsqrt(jnp.sum(ss, axis=-1, keepdims=True) * (1.0 / width) + EPS)
    gate = jnp.zeros((seqs, 128), F32)
    for k in range(kt):
        at = slice(k * 128, (k + 1) * 128)
        n = (mid[k].astype(F32) * scale * mgain[:, at]).astype(BF16)
        nmix[:, at] = n
        gate = gate + n.astype(F32) * bg[:, at]
    switch = jax.nn.sigmoid(jnp.sum(gate, axis=-1, keepdims=True))
    n = nmix[...]
    g = jnp.dot(n, sg[...], preferred_element_type=F32)
    u = jnp.dot(n, su[...], preferred_element_type=F32)
    hidden = (g * jax.nn.sigmoid(g) * u).astype(BF16)
    sout = jnp.dot(hidden, sd[...], preferred_element_type=F32)
    for k in range(kt):
        ssend[k] = sout[:, k * 128 : (k + 1) * 128].astype(BF16)
    put_tp(6, lambda f: ssend.at[f // 2], srecv)
    srecv[me_t] = ssend[my_k]

    for i in (14, 15, 16):
        copies[i].wait()
    arrived(4, ibox, ep_n - 1)
    for e in range(ep_n):
        xt[e : e + 1, :] = ibox[e, :, 0:128]
        xt[ep_n + e : ep_n + e + 1, :] = ibox[e, :, 128:256]
    xg[my_k] = xt[...].astype(BF16)
    put_tiles(7, xg)
    arrived(7, xg, 2 * yn - 1)
    ss = jnp.zeros((2 * ep_n, 128), F32)
    for k in range(kt):
        m = xg[k].astype(F32)
        ss = ss + m * m
    scale = lax.rsqrt(jnp.sum(ss, axis=-1, keepdims=True) * (1.0 / width) + EPS)
    for k in range(kt):
        at = slice(k * 128, (k + 1) * 128)
        xn[:, at] = (xg[k].astype(F32) * scale * mgain[:, at]).astype(BF16)
    x = xn[...]
    g = jnp.dot(x, eg[...], preferred_element_type=F32)
    u = jnp.dot(x, eu[...], preferred_element_type=F32)
    hidden = (g * jax.nn.sigmoid(g) * u).astype(BF16)
    lane = lax.broadcasted_iota(jnp.int32, (ep_n, 128), 1)
    for k in range(kt):
        at = slice(k * 128, (k + 1) * 128)
        out = jnp.dot(hidden, ed[:, at], preferred_element_type=F32)
        first, second = out[:ep_n], out[ep_n:]
        esend[2 * k] = jnp.where(lane < 64, first, pltpu.roll(second, 64, 1)).astype(BF16)
        esend[2 * k + 1] = jnp.where(lane < 64, pltpu.roll(first, 64, 1), second).astype(BF16)
    put_tp(8, lambda f: esend.at[f], erecv)
    erecv[me_t] = esend[me_t]
    arrived(6, srecv, tp_n - 1)
    base = middle + switch * jnp.sum(srecv[...].astype(F32), axis=0)
    base = jnp.where(side == 1, pltpu.roll(base, 64, 1), base)
    arrived(8, erecv, tp_n - 1)
    total = erecv[0].astype(F32)
    for j in range(1, tp_n):
        total = total + erecv[j].astype(F32)
    for e in range(ep_n):
        rsend[e] = total[e : e + 1, :]
    put_ep(9, lambda f: rsend.at[f], rrecv)
    rrecv[me_e] = rsend[me_e]
    arrived(9, rrecv, ep_n - 1)
    row = lax.broadcasted_iota(jnp.int32, (seqs, 128), 0)
    routed = jnp.zeros((seqs, 128), F32)
    for b in range(seqs):
        line = jnp.zeros((1, 128), F32)
        for k in range(2):
            got = rrecv[ids[2 * b + k]]
            got = jnp.where(places[2 * b + k] == 1, pltpu.roll(got, 64, 1), got)
            line = line + rweights[b, k] * got
        routed = jnp.where(row == b, line, routed)
    mixed_out[...] = (base + routed)[:, :64].astype(BF16)

    sent(0, nrecv, ep_n - 1)
    sent(1, qrecv, ep_n - 1)
    sent(2, kvrecv, ep_n - 1)
    sent(3, arecv, tp_n - 1)
    sent(4, ibox, ep_n - 1)
    sent(5, mid, 2 * yn - 1)
    sent(6, srecv, tp_n - 1)
    sent(7, xg, 2 * yn - 1)
    sent(8, erecv, tp_n - 1)
    sent(9, rrecv, ep_n - 1)


def body(
    ep_n,
    tp_n,
    tokens,
    attn_gain,
    query_weight,
    key_weight,
    value_weight,
    query_gain,
    stick_bias,
    key_cache,
    value_cache,
    lengths,
    out_weight,
    mix_gain,
    route_ids,
    route_weights,
    expert_gate,
    expert_up,
    expert_down,
    side_gate,
    side_up,
    side_down,
    branch_gate,
):
    seqs, width = tokens.shape
    slots = key_cache.shape[2]
    kt = width // 128
    any_ = pl.BlockSpec(memory_space=pl.ANY)
    smem = pl.BlockSpec(memory_space=pltpu.SMEM)
    vmem = pl.BlockSpec(memory_space=pltpu.VMEM)
    specs = [any_] * 21
    for i in (6, 9, 12, 13):
        specs[i] = smem
    V = pltpu.VMEM
    scratch = [
        V((seqs, width), BF16),
        V((1, width), F32),
        V((1, width), F32),
        V((1, DH), F32),
        V((1, width), F32),
        V((2 * query_weight.shape[0], 3 * DH), BF16),
        V((seqs, slots, DH), BF16),
        V((seqs, slots, DH), BF16),
        V(out_weight.shape, BF16),
        V(expert_gate.shape[1:], BF16),
        V(expert_up.shape[1:], BF16),
        V(expert_down.shape[1:], BF16),
        V(side_gate.shape, BF16),
        V(side_up.shape, BF16),
        V(side_down.shape, BF16),
        V((slots, slots), BF16),
        V((kt, seqs, 128), F32),
        V((kt, seqs, 128), BF16),
        V((ep_n, seqs, 128), BF16),
        V((ep_n, seqs, 128), BF16),
        V((ep_n, seqs, 128), BF16),
        V((ep_n, 2, seqs, 128), BF16),
        V((ep_n, 2, seqs, 128), BF16),
        V((kt, seqs, 128), BF16),
        V((tp_n, seqs, 128), BF16),
        V((kt, seqs, 128), BF16),
        V((seqs, width), BF16),
        V((2 * ep_n, 128), F32),
        V((ep_n, 1, 256), F32),
        V((ep_n, 1, 256), F32),
        V((2 * ep_n, 128), F32),
        V((kt, 2 * ep_n, 128), BF16),
        V((2 * ep_n, width), BF16),
        V((kt, seqs, 128), BF16),
        V((tp_n, seqs, 128), BF16),
        V((tp_n, ep_n, 128), BF16),
        V((tp_n, ep_n, 128), BF16),
        V((ep_n, 1, 128), F32),
        V((ep_n, 1, 128), F32),
        pltpu.SemaphoreType.DMA((17,)),
        pltpu.SemaphoreType.DMA((10,)),
        pltpu.SemaphoreType.DMA((10,)),
    ]
    return pl.pallas_call(
        functools.partial(kernel, ep_n, tp_n),
        out_shape=(
            jax.ShapeDtypeStruct((seqs, width // tp_n), BF16),
            jax.ShapeDtypeStruct((seqs, DH), BF16),
            jax.ShapeDtypeStruct((seqs, DH), BF16),
        ),
        in_specs=specs,
        out_specs=(vmem, vmem, vmem),
        scratch_shapes=scratch,
        compiler_params=pltpu.CompilerParams(
            collective_id=0, has_side_effects=True, vmem_limit_bytes=60 * 1024 * 1024
        ),
        name="decode_layer",
    )(
        tokens,
        attn_gain.reshape(1, -1),
        query_weight,
        key_weight,
        value_weight,
        query_gain.reshape(1, -1),
        stick_bias,
        key_cache,
        value_cache,
        lengths,
        out_weight,
        mix_gain.reshape(1, -1),
        route_ids,
        route_weights,
        expert_gate,
        expert_up,
        expert_down,
        side_gate,
        side_up,
        side_down,
        branch_gate.reshape(1, -1),
    )


def solution(mesh):
    in_specs = (
        P("ep", None),
        P(),
        P("ep", "tp"),
        P("ep", "tp"),
        P("ep", "tp"),
        P(),
        P("tp"),
        P("ep", "tp", None, None),
        P("ep", "tp", None, None),
        P("ep"),
        P("tp", None),
        P(),
        P("ep", None),
        P("ep", None),
        P("ep", None, "tp"),
        P("ep", None, "tp"),
        P("ep", "tp", None),
        P(None, "tp"),
        P(None, "tp"),
        P("tp", None),
        P(),
    )
    out_specs = (P("ep", "tp"), P("ep", "tp"), P("ep", "tp"))
    step = functools.partial(body, mesh.shape["ep"], mesh.shape["tp"])
    return jax.shard_map(step, mesh=mesh, in_specs=in_specs, out_specs=out_specs, check_vma=False)
```

```python
import functools

import jax
import jax.numpy as jnp
from jax import lax
from jax.experimental import pallas as pl
from jax.experimental.pallas import tpu as pltpu
from jax.sharding import PartitionSpec as P

DH = 128
XN = 4
EPS = 1e-06
F32 = jnp.float32
BF16 = jnp.bfloat16
MESH = pl.DeviceIdType.MESH


def far_first(i, n):
    half = (i + 1) // 2
    return n // 2 - half * (2 * lax.rem(i + 1, 2) - 1)


def dot_t(a, b):
    return lax.dot_general(a, b, (((1,), (1,)), ((), ())), preferred_element_type=F32)


def log_sigmoids(x):
    t = jnp.log1p(jnp.exp(-jnp.abs(x)))
    return jnp.minimum(x, 0.0) - t, jnp.minimum(-x, 0.0) - t


def kernel(
    ep_n,
    tp_n,
    tokens,
    attn_gain,
    wq,
    wk,
    wv,
    qgain,
    bias,
    kcache,
    vcache,
    lengths_in,
    oweight,
    mix_gain,
    rids_in,
    rweights_in,
    egate,
    eup,
    edown,
    sgate,
    sup,
    sdown,
    bgate,
    mixed_out,
    keys_out,
    values_out,
    tok,
    again,
    mgain,
    qg,
    bg,
    wpad,
    kb,
    vb,
    ow,
    eg,
    eu,
    ed,
    sg,
    su,
    sd,
    tri,
    tiles,
    nsend,
    nrecv,
    kvsend,
    kvrecv,
    asend,
    arecv,
    mid,
    nmix,
    xo,
    obox,
    ibox,
    xt,
    xg,
    xn,
    ssend,
    srecv,
    esend,
    erecv,
    rsend,
    rrecv,
    wall,
    lengths,
    rids,
    rweights,
    far,
    parts,
    back,
    ld,
    snd,
    rcv,
    wsnd,
    wrcv,
):
    me_e = lax.axis_index("ep")
    me_t = lax.axis_index("tp")
    core = lax.rem(me_e, 2)
    yn = tp_n // XN
    my_y = me_t // XN
    my_x = lax.rem(me_t, XN)
    my_k = me_t // 2
    side = lax.rem(me_t, 2)
    kt = tp_n // 2
    seqs, width = tok.shape
    slots = kb.shape[1]

    def ep_peer(i):
        return lax.rem(me_e + far_first(i, ep_n), ep_n)

    def tp_peer(i):
        dy = far_first(i // XN, yn)
        dx = far_first(lax.rem(i, XN), XN)
        return lax.rem(my_y + dy, yn) * XN + lax.rem(my_x + dx, XN)

    barrier = pltpu.get_barrier_semaphore()

    def along(k):
        return lax.rem(me_e + 2 * k + ep_n, ep_n)

    def tell(sem, dest):
        pl.semaphore_signal(sem, inc=1, device_id=dest, device_id_type=MESH)

    near = ep_n // 8
    zs = ep_n // 2
    my_z = me_e // 2
    partner = {"ep": me_e + 1 - 2 * core}

    def greet_ep(i, c):
        tell(barrier, {"ep": ep_peer(i)})
        return c

    def greet_tp(i, c):
        tell(barrier, {"tp": tp_peer(i)})
        return c

    lax.fori_loop(0, ep_n - 1, greet_ep, 0)
    lax.fori_loop(0, tp_n - 1, greet_tp, 0)

    rows_w = wq.shape[0]
    at_w = pl.ds(pl.multiple_of(core * rows_w, rows_w), rows_w)
    loads = [
        (tokens, tok),
        (attn_gain, again),
        (wq, wall.at[me_e]),
        (wk, wpad.at[at_w, pl.ds(0, DH)]),
        (wv, wpad.at[at_w, pl.ds(DH, DH)]),
        (qgain, qg),
        (kcache.at[:, 0], kb),
        (vcache.at[:, 0], vb),
        (oweight, ow),
        (mix_gain, mgain),
        (bgate, bg),
        (sgate, sg),
        (sup, su),
        (sdown, sd),
        (egate.at[0], eg),
        (eup.at[0], eu),
        (edown.at[0], ed),
        (lengths_in, lengths),
        (rids_in, rids),
        (rweights_in, rweights),
    ]
    copies = [pltpu.make_async_copy(a, b, ld.at[i]) for i, (a, b) in enumerate(loads)]
    for i in (2, 0, 1):
        copies[i].start()
    for i, c in enumerate(copies):
        if i > 2:
            c.start()

    other = pl.ds(pl.multiple_of((1 - core) * rows_w, rows_w), rows_w)
    wpad[other, :] = jnp.zeros((rows_w, 2 * DH), BF16)
    r_i = lax.broadcasted_iota(jnp.int32, (slots, slots), 0)
    c_i = lax.broadcasted_iota(jnp.int32, (slots, slots), 1)
    tri[...] = jnp.where(r_i > c_i, 1.0, 0.0).astype(BF16)

    copies[0].wait()
    copies[1].wait()
    stream = tok[...].astype(F32)
    ms = jnp.mean(stream * stream, axis=-1, keepdims=True)
    normed = (stream * lax.rsqrt(ms + EPS) * again[...]).astype(BF16)
    for k in range(kt):
        tiles[k] = stream[:, k * 128 : (k + 1) * 128]
        nsend[k] = normed[:, k * 128 : (k + 1) * 128]
    nrecv[me_e] = nsend[me_e // 2]
    copies[2].wait()
    pl.semaphore_wait(barrier, ep_n + tp_n - 2)

    def put_block(dest, block, p, sem):
        pltpu.make_async_remote_copy(
            src_ref=wall.at[block],
            dst_ref=wall.at[block],
            send_sem=wsnd.at[p],
            recv_sem=sem,
            device_id=dest,
            device_id_type=MESH,
        ).start()

    def chip_at(d):
        return lax.rem(my_z + d + zs, zs)

    def put_far(dest, d, slot):
        pltpu.make_async_remote_copy(
            src_ref=nsend.at[chip_at(d)],
            dst_ref=far.at[slot],
            send_sem=snd.at[1],
            recv_sem=rcv.at[1],
            device_id={"ep": dest},
            device_id_type=MESH,
        ).start()

    for k in range(near, 0, -1):
        put_block({"ep": along(-k)}, me_e, 0, wrcv.at[me_e])
        put_block({"ep": along(k)}, me_e, 0, wrcv.at[me_e])
        if k == near:
            put_block(partner, me_e, 1, wrcv.at[ep_n])
            for d in range(1, near + 1):
                put_far(along(near), near + d, d - 1)
            for d in range(1, near):
                put_far(along(-near), -near - d, near + d - 1)

    def put_ep(p, src_of, dst, first=0, end=ep_n - 1, place=lambda i: me_e, peer=ep_peer):
        def one(i, c):
            f = peer(i)
            pltpu.make_async_remote_copy(
                src_ref=src_of(f),
                dst_ref=dst.at[place(i)],
                send_sem=snd.at[p],
                recv_sem=rcv.at[p],
                device_id={"ep": f},
                device_id_type=MESH,
            ).start()
            return c

        lax.fori_loop(first, end, one, 0)

    def put_tp(p, src_of, dst):
        def one(i, c):
            f = tp_peer(i)
            pltpu.make_async_remote_copy(
                src_ref=src_of(f),
                dst_ref=dst.at[me_t],
                send_sem=snd.at[p],
                recv_sem=rcv.at[p],
                device_id={"tp": f},
                device_id_type=MESH,
            ).start()
            return c

        lax.fori_loop(0, tp_n - 1, one, 0)

    def put_tiles(p, buf):
        def one(i, c):
            q = lax.rem(i + 1, 2)
            y = lax.rem(my_y + far_first(i // 2, yn), yn)
            f = y * XN + q * (XN - 1 - my_x) + (1 - q) * my_x
            pltpu.make_async_remote_copy(
                src_ref=buf.at[my_k],
                dst_ref=buf.at[my_k],
                send_sem=snd.at[p],
                recv_sem=rcv.at[p],
                device_id={"tp": f},
                device_id_type=MESH,
            ).start()
            return c

        lax.fori_loop(0, 2 * yn - 1, one, 0)

    def arrived(p, buf, n):
        part = buf.at[pl.ds(0, n)]
        pltpu.make_async_copy(part, part, rcv.at[p]).wait()

    def sent(p, buf, n):
        part = buf.at[pl.ds(0, n)]
        pltpu.make_async_copy(part, part, snd.at[p]).wait()

    for i in (17, 18, 19):
        copies[i].wait()
    ids = [rids[k, b] for b in range(seqs) for k in range(2)]
    places = []
    for i in range(2 * seqs):
        n = jnp.int32(0)
        for j in range(i):
            if j // 2 != i // 2:
                n = n + jnp.where(ids[j] == ids[i], 1, 0)
        places.append(n)

    row = lax.broadcasted_iota(jnp.int32, (seqs, slots), 0)
    pos = lax.broadcasted_iota(jnp.int32, (seqs, slots), 1)
    lens = jnp.zeros((seqs, slots), jnp.int32)
    for b in range(seqs):
        lens = jnp.where(row == b, lengths[b], lens)
    visible = pos < lens
    for i in (5, 6, 7, 8):
        copies[i].wait()

    def block_came(block):
        pltpu.make_async_copy(wall.at[block], wall.at[block], wrcv.at[block]).wait()
        put_block(partner, block, 1, wrcv.at[ep_n])

    for k in range(1, near + 1):
        block_came(along(-k))
        block_came(along(k))
    arrived(1, far, 2 * near - 1)
    theirs = wall.at[pl.ds(0, 2 * near + 1)]
    pltpu.make_async_copy(theirs, theirs, wrcv.at[ep_n]).wait()

    def times_block(rows, d):
        block = wall[pl.ds(2 * chip_at(d), 2)].reshape(128, DH)
        return jnp.dot(rows, block, preferred_element_type=F32)

    q = times_block(nsend[chip_at(0)], 0)
    from_low = jnp.zeros((seqs, DH), F32)
    from_high = jnp.zeros((seqs, DH), F32)
    for d in range(1, near + 1):
        both = jnp.concatenate([nsend[chip_at(d)], far[d - 1]], axis=0)
        both = times_block(both, d)
        q = q + both[:seqs]
        from_low = from_low + both[seqs:]
        if d < near:
            both = jnp.concatenate([nsend[chip_at(-d)], far[near + d - 1]], axis=0)
            both = times_block(both, -d)
            q = q + both[:seqs]
            from_high = from_high + both[seqs:]
        else:
            q = q + times_block(nsend[chip_at(-d)], -d)
    parts[0] = from_low
    parts[1] = from_high

    def put_part(dest, slot):
        pltpu.make_async_remote_copy(
            src_ref=parts.at[slot],
            dst_ref=back.at[slot],
            send_sem=wsnd.at[2],
            recv_sem=wrcv.at[ep_n + 1],
            device_id={"ep": dest},
            device_id_type=MESH,
        ).start()

    put_part(along(-near), 0)
    put_part(along(near), 1)
    pltpu.make_async_copy(back, back, wrcv.at[ep_n + 1]).wait()
    q = q + back[0] + back[1]
    q = q.astype(BF16).astype(F32)
    ms = jnp.mean(q * q, axis=-1, keepdims=True)
    q = (q * lax.rsqrt(ms + EPS) * qg[...]).astype(BF16)
    scores = jnp.zeros((seqs, slots), F32)
    for b in range(seqs):
        s = dot_t(q, kb[b])
        scores = jnp.where(row == b, s, scores)
    scores = scores * DH ** (-0.5) + bias[0]
    take, rest = log_sigmoids(scores)
    rest = jnp.where(visible, rest, 0.0)
    hi = rest.astype(BF16)
    left = rest - hi.astype(F32)
    lo = left.astype(BF16)
    last = (left - lo.astype(F32)).astype(BF16)
    t = tri[...]
    between = (
        jnp.dot(hi, t, preferred_element_type=F32)
        + jnp.dot(lo, t, preferred_element_type=F32)
        + jnp.dot(last, t, preferred_element_type=F32)
    )
    stick = jnp.where(visible, jnp.exp(take + between), 0.0)
    att = jnp.zeros((seqs, DH), F32)
    for b in range(seqs):
        only = jnp.where(row == b, stick, 0.0).astype(BF16)
        att = att + jnp.dot(only, vb[b], preferred_element_type=F32)
    att = att.astype(BF16)
    proj = jnp.dot(att, ow[...], preferred_element_type=F32)
    for k in range(kt):
        asend[k] = proj[:, k * 128 : (k + 1) * 128].astype(BF16)
    put_tp(3, lambda f: asend.at[f // 2], arecv)
    arecv[me_t] = asend[my_k]

    put_ep(0, lambda f: nsend.at[f // 2], nrecv)

    arrived(3, arecv, tp_n - 1)
    middle = (tiles[my_k] + jnp.sum(arecv[...].astype(F32), axis=0)).astype(BF16)
    mid[my_k] = middle
    middle = middle.astype(F32)
    slot_row = lax.broadcasted_iota(jnp.int32, (2 * ep_n, 128), 0)
    outbox = jnp.zeros((2 * ep_n, 128), F32)
    for i in range(2 * seqs):
        b = i // 2
        outbox = jnp.where(slot_row == places[i] * ep_n + ids[i], middle[b : b + 1, :], outbox)
    xo[...] = outbox
    for e in range(ep_n):
        obox[e, :, 0:128] = xo[e : e + 1, :]
        obox[e, :, 128:256] = xo[ep_n + e : ep_n + e + 1, :]
    half = ep_n // 2
    quarter = ep_n // 4

    def offset(i):
        return lax.rem(ep_n + quarter - far_first(i, ep_n), ep_n)

    put_ep(4, lambda f: obox.at[f], ibox, 0, half, offset)
    put_ep(10, lambda f: obox.at[f], ibox, half, ep_n - 1, offset)
    put_tiles(5, mid)
    ibox[quarter] = obox[me_e]

    for i in (9, 10, 11, 12, 13):
        copies[i].wait()
    arrived(5, mid, 2 * yn - 1)
    ss = jnp.zeros((seqs, 128), F32)
    for k in range(kt):
        m = mid[k].astype(F32)
        ss = ss + m * m
    scale = lax.rsqrt(jnp.sum(ss, axis=-1, keepdims=True) * (1.0 / width) + EPS)
    gate = jnp.zeros((seqs, 128), F32)
    for k in range(kt):
        at = slice(k * 128, (k + 1) * 128)
        n = (mid[k].astype(F32) * scale * mgain[:, at]).astype(BF16)
        nmix[:, at] = n
        gate = gate + n.astype(F32) * bg[:, at]
    switch = jax.nn.sigmoid(jnp.sum(gate, axis=-1, keepdims=True))
    n = nmix[...]
    g = dot_t(n, sg[...])
    u = dot_t(n, su[...])
    hidden = (g * jax.nn.sigmoid(g) * u).astype(BF16)
    sout = jnp.dot(hidden, sd[...], preferred_element_type=F32)
    for k in range(kt):
        ssend[k] = sout[:, k * 128 : (k + 1) * 128].astype(BF16)
    put_tp(6, lambda f: ssend.at[f // 2], srecv)
    srecv[me_t] = ssend[my_k]

    for i in (14, 15, 16):
        copies[i].wait()
    def pass_on(g, p):
        for r in range(half):
            xt[r : r + 1, :] = ibox[g * half + r, :, 0:128]
            xt[half + r : half + r + 1, :] = ibox[g * half + r, :, 128:256]
        xg[g, my_k] = xt[...].astype(BF16)
        put_tiles(p, xg.at[g])

    arrived(10, ibox, half - 1)
    pass_on(0, 7)
    arrived(4, ibox, half)
    pass_on(1, 11)

    copies[3].wait()
    copies[4].wait()
    arrived(0, nrecv, ep_n - 1)
    picked = nrecv[...].astype(F32).reshape(ep_n * seqs, 128).astype(BF16)
    part = jnp.dot(picked, wpad[...], preferred_element_type=F32)
    for f in range(ep_n):
        kvsend[f, 0] = part[f * seqs : (f + 1) * seqs, :DH].astype(BF16)
        kvsend[f, 1] = part[f * seqs : (f + 1) * seqs, DH:].astype(BF16)
    put_ep(2, lambda f: kvsend.at[f], kvrecv)
    kvrecv[me_e] = kvsend[me_e]

    lane = lax.broadcasted_iota(jnp.int32, (half, 128), 1)

    def expert(g, p, q):
        arrived(p, xg.at[g], 2 * yn - 1)
        ss = jnp.zeros((ep_n, 128), F32)
        for k in range(kt):
            m = xg[g, k].astype(F32)
            ss = ss + m * m
        scale = lax.rsqrt(jnp.sum(ss, axis=-1, keepdims=True) * (1.0 / width) + EPS)
        for k in range(kt):
            at = slice(k * 128, (k + 1) * 128)
            xn[:, at] = (xg[g, k].astype(F32) * scale * mgain[:, at]).astype(BF16)
        x = xn[...]
        a = dot_t(x, eg[...])
        u = dot_t(x, eu[...])
        hidden = (a * jax.nn.sigmoid(a) * u).astype(BF16)
        for k in range(kt):
            at = slice(k * 128, (k + 1) * 128)
            out = jnp.dot(hidden, ed[:, at], preferred_element_type=F32)
            top, low = out[:half], out[half:]
            esend[g, 2 * k] = jnp.where(lane < 64, top, pltpu.roll(low, 64, 1)).astype(BF16)
            esend[g, 2 * k + 1] = jnp.where(lane < 64, pltpu.roll(top, 64, 1), low).astype(BF16)
        put_tp(q, lambda f: esend.at[g, f], erecv.at[g])
        erecv[g, me_t] = esend[g, me_t]

    expert(0, 7, 8)
    expert(1, 11, 12)
    arrived(2, kvrecv, ep_n - 1)
    fresh = jnp.sum(kvrecv[:, 0].astype(F32), axis=0).astype(BF16).astype(F32)
    ms = jnp.mean(fresh * fresh, axis=-1, keepdims=True)
    keys_out[...] = (fresh * lax.rsqrt(ms + EPS)).astype(BF16)
    values_out[...] = jnp.sum(kvrecv[:, 1].astype(F32), axis=0).astype(BF16)

    arrived(6, srecv, tp_n - 1)
    base = middle + switch * jnp.sum(srecv[...].astype(F32), axis=0)
    base = jnp.where(side == 1, pltpu.roll(base, 64, 1), base)

    def give_back(g, p, first, end):
        arrived(p, erecv.at[g], tp_n - 1)
        total = erecv[g, 0].astype(F32)
        for j in range(1, tp_n):
            total = total + erecv[g, j].astype(F32)
        for r in range(half):
            rsend[g * half + r] = total[r : r + 1, :]

        def back_offset(f):
            return lax.rem(f - me_e + quarter + ep_n, ep_n)

        def source(i):
            return lax.rem(me_e + ep_n - far_first(i, ep_n), ep_n)

        put_ep(9, lambda f: rsend.at[back_offset(f)], rrecv, first, end, peer=source)

    give_back(0, 8, half, ep_n - 1)
    give_back(1, 12, 0, half)
    rrecv[me_e] = rsend[quarter]
    arrived(9, rrecv, ep_n - 1)
    row = lax.broadcasted_iota(jnp.int32, (seqs, 128), 0)
    routed = jnp.zeros((seqs, 128), F32)
    for b in range(seqs):
        line = jnp.zeros((1, 128), F32)
        for k in range(2):
            got = rrecv[ids[2 * b + k]]
            got = jnp.where(places[2 * b + k] == 1, pltpu.roll(got, 64, 1), got)
            line = line + rweights[k, b] * got
        routed = jnp.where(row == b, line, routed)
    mixed_out[...] = (base + routed)[:, :64].astype(BF16)

    sent(0, nrecv, ep_n - 1)
    sent(1, far, 2 * near - 1)
    others = wall.at[pl.ds(0, 2 * near)]
    pltpu.make_async_copy(others, others, wsnd.at[0]).wait()
    pltpu.make_async_copy(theirs, theirs, wsnd.at[1]).wait()
    pltpu.make_async_copy(back, back, wsnd.at[2]).wait()
    sent(2, kvrecv, ep_n - 1)
    sent(3, arecv, tp_n - 1)
    sent(4, ibox, half)
    sent(10, ibox, half - 1)
    sent(5, mid, 2 * yn - 1)
    sent(6, srecv, tp_n - 1)
    for g in range(2):
        sent((7, 11)[g], xg.at[g], 2 * yn - 1)
        sent((8, 12)[g], erecv.at[g], tp_n - 1)
    sent(9, rrecv, ep_n - 1)


def hand_over(a, b, c, x, y, z, sem):
    copies = [
        pltpu.make_async_copy(src, dst, sem.at[i])
        for i, (src, dst) in enumerate(((a, x), (b, y), (c, z)))
    ]
    for one in copies:
        one.start()
    for one in copies:
        one.wait()


def body(
    ep_n,
    tp_n,
    tokens,
    attn_gain,
    query_weight,
    key_weight,
    value_weight,
    query_gain,
    stick_bias,
    key_cache,
    value_cache,
    lengths,
    out_weight,
    mix_gain,
    route_ids,
    route_weights,
    expert_gate,
    expert_up,
    expert_down,
    side_gate,
    side_up,
    side_down,
    branch_gate,
):
    seqs, width = tokens.shape
    slots = key_cache.shape[2]
    kt = width // 128
    any_ = pl.BlockSpec(memory_space=pl.ANY)
    vmem = pl.BlockSpec(memory_space=pltpu.VMEM)
    specs = [any_] * 21
    specs[6] = pl.BlockSpec(memory_space=pltpu.SMEM)
    V = pltpu.VMEM
    scratch = [
        V((seqs, width), BF16),
        V((1, width), F32),
        V((1, width), F32),
        V((1, DH), F32),
        V((1, width), F32),
        V((2 * query_weight.shape[0], 2 * DH), BF16),
        V((seqs, slots, DH), BF16),
        V((seqs, slots, DH), BF16),
        V(out_weight.shape, BF16),
        V(expert_gate.shape[:0:-1], BF16),
        V(expert_up.shape[:0:-1], BF16),
        V(expert_down.shape[1:], BF16),
        V(side_gate.shape[::-1], BF16),
        V(side_up.shape[::-1], BF16),
        V(side_down.shape, BF16),
        V((slots, slots), BF16),
        V((kt, seqs, 128), F32),
        V((kt, seqs, 128), BF16),
        V((ep_n, seqs, 128), BF16),
        V((ep_n, 2, seqs, 128), BF16),
        V((ep_n, 2, seqs, 128), BF16),
        V((kt, seqs, 128), BF16),
        V((tp_n, seqs, 128), BF16),
        V((kt, seqs, 128), BF16),
        V((seqs, width), BF16),
        V((2 * ep_n, 128), F32),
        V((ep_n, 1, 256), F32),
        V((ep_n, 1, 256), F32),
        V((ep_n, 128), F32),
        V((2, kt, ep_n, 128), BF16),
        V((ep_n, width), BF16),
        V((kt, seqs, 128), BF16),
        V((tp_n, seqs, 128), BF16),
        V((2, tp_n, ep_n // 2, 128), BF16),
        V((2, tp_n, ep_n // 2, 128), BF16),
        V((ep_n, 1, 128), F32),
        V((ep_n, 1, 128), F32),
        V((ep_n, *query_weight.shape), BF16),
        pltpu.SMEM((seqs,), jnp.int32),
        pltpu.SMEM((2, seqs), jnp.int32),
        pltpu.SMEM((2, seqs), F32),
        V((ep_n // 4 - 1, seqs, 128), BF16),
        V((2, seqs, DH), F32),
        V((2, seqs, DH), F32),
        pltpu.SemaphoreType.DMA((20,)),
        pltpu.SemaphoreType.DMA((13,)),
        pltpu.SemaphoreType.DMA((13,)),
        pltpu.SemaphoreType.DMA((3,)),
        pltpu.SemaphoreType.DMA((ep_n + 2,)),
    ]
    shapes = ((seqs, width // tp_n), (seqs, DH), (seqs, DH))
    results = pl.pallas_call(
        functools.partial(kernel, ep_n, tp_n),
        out_shape=tuple(V(s, BF16) for s in shapes),
        in_specs=specs,
        out_specs=(vmem, vmem, vmem),
        scratch_shapes=scratch,
        compiler_params=pltpu.CompilerParams(
            collective_id=0, has_side_effects=True, vmem_limit_bytes=60 * 1024 * 1024
        ),
        name="decode_layer",
    )(
        tokens,
        attn_gain.reshape(1, -1),
        query_weight,
        key_weight,
        value_weight,
        query_gain.reshape(1, -1),
        stick_bias,
        key_cache,
        value_cache,
        lengths,
        out_weight,
        mix_gain.reshape(1, -1),
        route_ids.T,
        route_weights.T,
        jnp.swapaxes(expert_gate, 1, 2),
        jnp.swapaxes(expert_up, 1, 2),
        expert_down,
        side_gate.T,
        side_up.T,
        side_down,
        branch_gate.reshape(1, -1),
    )
    return pl.pallas_call(
        hand_over,
        out_shape=tuple(jax.ShapeDtypeStruct(s, BF16) for s in shapes),
        in_specs=[vmem] * 3,
        out_specs=[any_] * 3,
        scratch_shapes=[pltpu.SemaphoreType.DMA((3,))],
        name="hand_over",
    )(*[pltpu.with_memory_space_constraint(r, pltpu.VMEM) for r in results])


def solution(mesh):
    in_specs = (
        P("ep", None),
        P(),
        P("ep", "tp"),
        P("ep", "tp"),
        P("ep", "tp"),
        P(),
        P("tp"),
        P("ep", "tp", None, None),
        P("ep", "tp", None, None),
        P("ep"),
        P("tp", None),
        P(),
        P("ep", None),
        P("ep", None),
        P("ep", None, "tp"),
        P("ep", None, "tp"),
        P("ep", "tp", None),
        P(None, "tp"),
        P(None, "tp"),
        P("tp", None),
        P(),
    )
    out_specs = (P("ep", "tp"), P("ep", "tp"), P("ep", "tp"))
    step = functools.partial(body, mesh.shape["ep"], mesh.shape["tp"])
    return jax.shard_map(step, mesh=mesh, in_specs=in_specs, out_specs=out_specs, check_vma=False)
```

```python
import functools

import jax
import jax.numpy as jnp
from jax import lax
from jax.experimental import pallas as pl
from jax.experimental.pallas import tpu as pltpu
from jax.sharding import PartitionSpec as P

DH = 128
XN = 4
EPS = 1e-06
F32 = jnp.float32
BF16 = jnp.bfloat16
MESH = pl.DeviceIdType.MESH


def far_first(i, n):
    half = (i + 1) // 2
    return n // 2 - half * (2 * lax.rem(i + 1, 2) - 1)


def dot_t(a, b):
    return lax.dot_general(a, b, (((1,), (1,)), ((), ())), preferred_element_type=F32)


def log_sigmoids(x):
    t = jnp.log1p(jnp.exp(-jnp.abs(x)))
    return jnp.minimum(x, 0.0) - t, jnp.minimum(-x, 0.0) - t


def kernel(
    ep_n,
    tp_n,
    tokens,
    attn_gain,
    wq,
    wk,
    wv,
    qgain,
    bias,
    kcache,
    vcache,
    lengths_in,
    oweight,
    mix_gain,
    rids_in,
    rweights_in,
    egate,
    eup,
    edown,
    sgate,
    sup,
    sdown,
    bgate,
    mixed_out,
    keys_out,
    values_out,
    tok,
    again,
    mgain,
    qg,
    bg,
    wpad,
    kb,
    vb,
    ow,
    eg,
    eu,
    ed,
    sg,
    su,
    sd,
    tri,
    tiles,
    nsend,
    nrecv,
    kvsend,
    kvrecv,
    asend,
    arecv,
    mid,
    nmix,
    xo,
    obox,
    ibox,
    xt,
    xg,
    xn,
    ssend,
    srecv,
    esend,
    erecv,
    rsend,
    rrecv,
    wall,
    lengths,
    rids,
    rweights,
    far,
    parts,
    back,
    from_down,
    from_up,
    column_left,
    column_right,
    ld,
    snd,
    rcv,
    wsnd,
    wrcv,
):
    me_e = lax.axis_index("ep")
    me_t = lax.axis_index("tp")
    core = lax.rem(me_e, 2)
    yn = tp_n // XN
    my_y = me_t // XN
    my_x = lax.rem(me_t, XN)
    my_k = me_t // 2
    side = lax.rem(me_t, 2)
    kt = tp_n // 2
    seqs, width = tok.shape
    slots = kb.shape[1]

    def ep_peer(i):
        return lax.rem(me_e + far_first(i, ep_n), ep_n)

    def tp_peer(i):
        dy = far_first(i // XN, yn)
        dx = far_first(lax.rem(i, XN), XN)
        return lax.rem(my_y + dy, yn) * XN + lax.rem(my_x + dx, XN)

    barrier = pltpu.get_barrier_semaphore()

    def along(k):
        return lax.rem(me_e + 2 * k + ep_n, ep_n)

    def tell(sem, dest):
        pl.semaphore_signal(sem, inc=1, device_id=dest, device_id_type=MESH)

    near = ep_n // 8
    zs = ep_n // 2
    my_z = me_e // 2
    partner = {"ep": me_e + 1 - 2 * core}

    y_down = {"tp": lax.rem(my_y + yn - 1, yn) * XN + my_x}
    y_up = {"tp": lax.rem(my_y + 1, yn) * XN + my_x}
    x_left = {"tp": my_y * XN + lax.rem(my_x + XN - 1, XN)}
    x_right = {"tp": my_y * XN + lax.rem(my_x + 1, XN)}
    greeted = [partner, y_down, y_up, x_left, x_right]
    for k in range(near, 0, -1):
        greeted += [{"ep": along(-k)}, {"ep": along(k)}]
    for dest in greeted:
        tell(barrier, dest)

    rows_w = wq.shape[0]
    at_w = pl.ds(pl.multiple_of(core * rows_w, rows_w), rows_w)
    loads = [
        (tokens, tok),
        (attn_gain, again),
        (wq, wall.at[me_e]),
        (wk, wpad.at[at_w, pl.ds(0, DH)]),
        (wv, wpad.at[at_w, pl.ds(DH, DH)]),
        (qgain, qg),
        (kcache.at[:, 0], kb),
        (vcache.at[:, 0], vb),
        (oweight, ow),
        (mix_gain, mgain),
        (bgate, bg),
        (sgate, sg),
        (sup, su),
        (sdown, sd),
        (egate.at[0], eg),
        (eup.at[0], eu),
        (edown.at[0], ed),
        (lengths_in, lengths),
        (rids_in, rids),
        (rweights_in, rweights),
    ]
    copies = [pltpu.make_async_copy(a, b, ld.at[i]) for i, (a, b) in enumerate(loads)]
    for i in (2, 0, 1):
        copies[i].start()
    for i, c in enumerate(copies):
        if i > 2:
            c.start()

    other = pl.ds(pl.multiple_of((1 - core) * rows_w, rows_w), rows_w)
    wpad[other, :] = jnp.zeros((rows_w, 2 * DH), BF16)
    r_i = lax.broadcasted_iota(jnp.int32, (slots, slots), 0)
    c_i = lax.broadcasted_iota(jnp.int32, (slots, slots), 1)
    tri[...] = jnp.where(r_i > c_i, 1.0, 0.0).astype(BF16)

    copies[0].wait()
    copies[1].wait()
    stream = tok[...].astype(F32)
    ms = jnp.mean(stream * stream, axis=-1, keepdims=True)
    normed = (stream * lax.rsqrt(ms + EPS) * again[...]).astype(BF16)
    for k in range(kt):
        tiles[k] = stream[:, k * 128 : (k + 1) * 128]
        nsend[k] = normed[:, k * 128 : (k + 1) * 128]
    nrecv[me_e] = nsend[me_e // 2]
    copies[2].wait()
    pl.semaphore_wait(barrier, len(greeted))

    def put_block(dest, block, p, sem):
        pltpu.make_async_remote_copy(
            src_ref=wall.at[block],
            dst_ref=wall.at[block],
            send_sem=wsnd.at[p],
            recv_sem=sem,
            device_id=dest,
            device_id_type=MESH,
        ).start()

    def chip_at(d):
        return lax.rem(my_z + d + zs, zs)

    def put_far(dest, d, slot):
        pltpu.make_async_remote_copy(
            src_ref=nsend.at[chip_at(d)],
            dst_ref=far.at[slot],
            send_sem=snd.at[1],
            recv_sem=rcv.at[1],
            device_id={"ep": dest},
            device_id_type=MESH,
        ).start()

    for k in range(near, 0, -1):
        put_block({"ep": along(-k)}, me_e, 0, wrcv.at[me_e])
        put_block({"ep": along(k)}, me_e, 0, wrcv.at[me_e])
        if k == near:
            put_block(partner, me_e, 1, wrcv.at[ep_n])
            for d in range(1, near + 1):
                put_far(along(near), near + d, d - 1)
            for d in range(1, near):
                put_far(along(-near), -near - d, near + d - 1)

    tell(from_down.at[2], y_up)
    tell(from_up.at[2], y_down)
    for k in range(2, yn // 2 + 1):
        pl.semaphore_wait(from_down.at[k], 1)
        if k < yn // 2:
            tell(from_down.at[k + 1], y_up)
            pl.semaphore_wait(from_up.at[k], 1)
            if k < yn // 2 - 1:
                tell(from_up.at[k + 1], y_down)
    tell(column_left.at[0], x_right)
    tell(column_right.at[0], x_left)
    pl.semaphore_wait(column_left.at[0], 1)
    tell(column_left.at[1], x_right)
    pl.semaphore_wait(column_right.at[0], 1)
    pl.semaphore_wait(column_left.at[1], 1)

    def put_ep(p, src_of, dst, first=0, end=ep_n - 1, place=lambda i: me_e, peer=ep_peer):
        def one(i, c):
            f = peer(i)
            pltpu.make_async_remote_copy(
                src_ref=src_of(f),
                dst_ref=dst.at[place(i)],
                send_sem=snd.at[p],
                recv_sem=rcv.at[p],
                device_id={"ep": f},
                device_id_type=MESH,
            ).start()
            return c

        lax.fori_loop(first, end, one, 0)

    def put_tp(p, src_of, dst):
        def one(i, c):
            f = tp_peer(i)
            pltpu.make_async_remote_copy(
                src_ref=src_of(f),
                dst_ref=dst.at[me_t],
                send_sem=snd.at[p],
                recv_sem=rcv.at[p],
                device_id={"tp": f},
                device_id_type=MESH,
            ).start()
            return c

        lax.fori_loop(0, tp_n - 1, one, 0)

    def put_tiles(p, buf):
        def one(i, c):
            q = lax.rem(i + 1, 2)
            y = lax.rem(my_y + far_first(i // 2, yn), yn)
            f = y * XN + q * (XN - 1 - my_x) + (1 - q) * my_x
            pltpu.make_async_remote_copy(
                src_ref=buf.at[my_k],
                dst_ref=buf.at[my_k],
                send_sem=snd.at[p],
                recv_sem=rcv.at[p],
                device_id={"tp": f},
                device_id_type=MESH,
            ).start()
            return c

        lax.fori_loop(0, 2 * yn - 1, one, 0)

    def arrived(p, buf, n):
        part = buf.at[pl.ds(0, n)]
        pltpu.make_async_copy(part, part, rcv.at[p]).wait()

    def sent(p, buf, n):
        part = buf.at[pl.ds(0, n)]
        pltpu.make_async_copy(part, part, snd.at[p]).wait()

    for i in (17, 18, 19):
        copies[i].wait()
    ids = [rids[k, b] for b in range(seqs) for k in range(2)]
    places = []
    for i in range(2 * seqs):
        n = jnp.int32(0)
        for j in range(i):
            if j // 2 != i // 2:
                n = n + jnp.where(ids[j] == ids[i], 1, 0)
        places.append(n)

    row = lax.broadcasted_iota(jnp.int32, (seqs, slots), 0)
    pos = lax.broadcasted_iota(jnp.int32, (seqs, slots), 1)
    lens = jnp.zeros((seqs, slots), jnp.int32)
    for b in range(seqs):
        lens = jnp.where(row == b, lengths[b], lens)
    visible = pos < lens
    for i in (5, 6, 7, 8):
        copies[i].wait()

    def block_came(block):
        pltpu.make_async_copy(wall.at[block], wall.at[block], wrcv.at[block]).wait()
        put_block(partner, block, 1, wrcv.at[ep_n])

    for k in range(1, near + 1):
        block_came(along(-k))
        block_came(along(k))
    arrived(1, far, 2 * near - 1)
    theirs = wall.at[pl.ds(0, 2 * near + 1)]
    pltpu.make_async_copy(theirs, theirs, wrcv.at[ep_n]).wait()

    def times_block(rows, d):
        block = wall[pl.ds(2 * chip_at(d), 2)].reshape(128, DH)
        return jnp.dot(rows, block, preferred_element_type=F32)

    q = times_block(nsend[chip_at(0)], 0)
    from_low = jnp.zeros((seqs, DH), F32)
    from_high = jnp.zeros((seqs, DH), F32)
    for d in range(1, near + 1):
        both = jnp.concatenate([nsend[chip_at(d)], far[d - 1]], axis=0)
        both = times_block(both, d)
        q = q + both[:seqs]
        from_low = from_low + both[seqs:]
        if d < near:
            both = jnp.concatenate([nsend[chip_at(-d)], far[near + d - 1]], axis=0)
            both = times_block(both, -d)
            q = q + both[:seqs]
            from_high = from_high + both[seqs:]
        else:
            q = q + times_block(nsend[chip_at(-d)], -d)
    parts[0] = from_low
    parts[1] = from_high

    def put_part(dest, slot):
        pltpu.make_async_remote_copy(
            src_ref=parts.at[slot],
            dst_ref=back.at[slot],
            send_sem=wsnd.at[2],
            recv_sem=wrcv.at[ep_n + 1],
            device_id={"ep": dest},
            device_id_type=MESH,
        ).start()

    put_part(along(-near), 0)
    put_part(along(near), 1)
    pltpu.make_async_copy(back, back, wrcv.at[ep_n + 1]).wait()
    q = q + back[0] + back[1]
    q = q.astype(BF16).astype(F32)
    ms = jnp.mean(q * q, axis=-1, keepdims=True)
    q = (q * lax.rsqrt(ms + EPS) * qg[...]).astype(BF16)
    scores = jnp.zeros((seqs, slots), F32)
    for b in range(seqs):
        s = dot_t(q, kb[b])
        scores = jnp.where(row == b, s, scores)
    scores = scores * DH ** (-0.5) + bias[0]
    take, rest = log_sigmoids(scores)
    rest = jnp.where(visible, rest, 0.0)
    hi = rest.astype(BF16)
    left = rest - hi.astype(F32)
    lo = left.astype(BF16)
    last = (left - lo.astype(F32)).astype(BF16)
    pieces = jnp.concatenate([hi.astype(F32), lo.astype(F32), last.astype(F32)], axis=0)
    sums = jnp.dot(pieces.astype(BF16), tri[...], preferred_element_type=F32)
    between = sums[:seqs] + sums[seqs : 2 * seqs] + sums[2 * seqs :]
    stick = jnp.where(visible, jnp.exp(take + between), 0.0)
    att = jnp.zeros((seqs, DH), F32)
    for b in range(seqs):
        only = jnp.where(row == b, stick, 0.0).astype(BF16)
        att = att + jnp.dot(only, vb[b], preferred_element_type=F32)
    att = att.astype(BF16)
    proj = jnp.dot(att, ow[...], preferred_element_type=F32)
    for k in range(kt):
        asend[k] = proj[:, k * 128 : (k + 1) * 128].astype(BF16)
    put_tp(3, lambda f: asend.at[f // 2], arecv)
    arecv[me_t] = asend[my_k]

    put_ep(0, lambda f: nsend.at[f // 2], nrecv)

    arrived(3, arecv, tp_n - 1)
    middle = (tiles[my_k] + jnp.sum(arecv[...].astype(F32), axis=0)).astype(BF16)
    mid[my_k] = middle
    middle = middle.astype(F32)
    slot_row = lax.broadcasted_iota(jnp.int32, (2 * ep_n, 128), 0)
    outbox = jnp.zeros((2 * ep_n, 128), F32)
    for i in range(2 * seqs):
        b = i // 2
        outbox = jnp.where(slot_row == places[i] * ep_n + ids[i], middle[b : b + 1, :], outbox)
    xo[...] = outbox
    for e in range(ep_n):
        obox[e, :, 0:128] = xo[e : e + 1, :]
        obox[e, :, 128:256] = xo[ep_n + e : ep_n + e + 1, :]
    half = ep_n // 2
    quarter = ep_n // 4

    def offset(i):
        return lax.rem(ep_n + quarter - far_first(i, ep_n), ep_n)

    put_ep(4, lambda f: obox.at[f], ibox, 0, half, offset)
    put_ep(10, lambda f: obox.at[f], ibox, half, ep_n - 1, offset)
    put_tiles(5, mid)
    ibox[quarter] = obox[me_e]

    copies[3].wait()
    copies[4].wait()
    arrived(0, nrecv, ep_n - 1)
    picked = nrecv[...].astype(F32).reshape(ep_n * seqs, 128).astype(BF16)
    part = jnp.dot(picked, wpad[...], preferred_element_type=F32)
    for f in range(ep_n):
        kvsend[f, 0] = part[f * seqs : (f + 1) * seqs, :DH].astype(BF16)
        kvsend[f, 1] = part[f * seqs : (f + 1) * seqs, DH:].astype(BF16)

    def pass_on(g, p):
        for r in range(half):
            xt[r : r + 1, :] = ibox[g * half + r, :, 0:128]
            xt[half + r : half + r + 1, :] = ibox[g * half + r, :, 128:256]
        xg[g, my_k] = xt[...].astype(BF16)
        put_tiles(p, xg.at[g])

    arrived(10, ibox, half - 1)
    pass_on(0, 7)
    arrived(4, ibox, half)
    pass_on(1, 11)

    for i in (9, 10, 11, 12, 13):
        copies[i].wait()
    arrived(5, mid, 2 * yn - 1)
    ss = jnp.zeros((seqs, 128), F32)
    for k in range(kt):
        m = mid[k].astype(F32)
        ss = ss + m * m
    scale = lax.rsqrt(jnp.sum(ss, axis=-1, keepdims=True) * (1.0 / width) + EPS)
    gate = jnp.zeros((seqs, 128), F32)
    for k in range(kt):
        at = slice(k * 128, (k + 1) * 128)
        n = (mid[k].astype(F32) * scale * mgain[:, at]).astype(BF16)
        nmix[:, at] = n
        gate = gate + n.astype(F32) * bg[:, at]
    switch = jax.nn.sigmoid(jnp.sum(gate, axis=-1, keepdims=True))
    n = nmix[...]
    g = dot_t(n, sg[...])
    u = dot_t(n, su[...])
    hidden = (g * jax.nn.sigmoid(g) * u).astype(BF16)
    sout = jnp.dot(hidden, sd[...], preferred_element_type=F32)
    for k in range(kt):
        ssend[k] = sout[:, k * 128 : (k + 1) * 128].astype(BF16)
    put_tp(6, lambda f: ssend.at[f // 2], srecv)
    srecv[me_t] = ssend[my_k]
    put_ep(2, lambda f: kvsend.at[f], kvrecv)
    kvrecv[me_e] = kvsend[me_e]

    for i in (14, 15, 16):
        copies[i].wait()
    lane = lax.broadcasted_iota(jnp.int32, (half, 128), 1)

    def expert(g, p, q):
        arrived(p, xg.at[g], 2 * yn - 1)
        ss = jnp.zeros((ep_n, 128), F32)
        for k in range(kt):
            m = xg[g, k].astype(F32)
            ss = ss + m * m
        scale = lax.rsqrt(jnp.sum(ss, axis=-1, keepdims=True) * (1.0 / width) + EPS)
        for k in range(kt):
            at = slice(k * 128, (k + 1) * 128)
            xn[:, at] = (xg[g, k].astype(F32) * scale * mgain[:, at]).astype(BF16)
        x = xn[...]
        a = dot_t(x, eg[...])
        u = dot_t(x, eu[...])
        hidden = (a * jax.nn.sigmoid(a) * u).astype(BF16)
        for k in range(kt):
            at = slice(k * 128, (k + 1) * 128)
            out = jnp.dot(hidden, ed[:, at], preferred_element_type=F32)
            top, low = out[:half], out[half:]
            esend[g, 2 * k] = jnp.where(lane < 64, top, pltpu.roll(low, 64, 1)).astype(BF16)
            esend[g, 2 * k + 1] = jnp.where(lane < 64, pltpu.roll(top, 64, 1), low).astype(BF16)
        put_tp(q, lambda f: esend.at[g, f], erecv.at[g])
        erecv[g, me_t] = esend[g, me_t]

    expert(0, 7, 8)
    expert(1, 11, 12)
    arrived(2, kvrecv, ep_n - 1)
    fresh = jnp.sum(kvrecv[:, 0].astype(F32), axis=0).astype(BF16).astype(F32)
    ms = jnp.mean(fresh * fresh, axis=-1, keepdims=True)
    keys_out[...] = (fresh * lax.rsqrt(ms + EPS)).astype(BF16)
    values_out[...] = jnp.sum(kvrecv[:, 1].astype(F32), axis=0).astype(BF16)

    arrived(6, srecv, tp_n - 1)
    base = middle + switch * jnp.sum(srecv[...].astype(F32), axis=0)
    base = jnp.where(side == 1, pltpu.roll(base, 64, 1), base)

    def give_back(g, p, first, end):
        arrived(p, erecv.at[g], tp_n - 1)
        total = erecv[g, 0].astype(F32)
        for j in range(1, tp_n):
            total = total + erecv[g, j].astype(F32)
        for r in range(half):
            rsend[g * half + r] = total[r : r + 1, :]

        def back_offset(f):
            return lax.rem(f - me_e + quarter + ep_n, ep_n)

        def source(i):
            return lax.rem(me_e + ep_n - far_first(i, ep_n), ep_n)

        put_ep(9, lambda f: rsend.at[back_offset(f)], rrecv, first, end, peer=source)

    give_back(0, 8, half, ep_n - 1)
    give_back(1, 12, 0, half)
    rrecv[me_e] = rsend[quarter]
    arrived(9, rrecv, ep_n - 1)
    row = lax.broadcasted_iota(jnp.int32, (seqs, 128), 0)
    routed = jnp.zeros((seqs, 128), F32)
    for b in range(seqs):
        line = jnp.zeros((1, 128), F32)
        for k in range(2):
            got = rrecv[ids[2 * b + k]]
            got = jnp.where(places[2 * b + k] == 1, pltpu.roll(got, 64, 1), got)
            line = line + rweights[k, b] * got
        routed = jnp.where(row == b, line, routed)
    mixed_out[...] = (base + routed)[:, :64].astype(BF16)

    sent(0, nrecv, ep_n - 1)
    sent(1, far, 2 * near - 1)
    others = wall.at[pl.ds(0, 2 * near)]
    pltpu.make_async_copy(others, others, wsnd.at[0]).wait()
    pltpu.make_async_copy(theirs, theirs, wsnd.at[1]).wait()
    pltpu.make_async_copy(back, back, wsnd.at[2]).wait()
    sent(2, kvrecv, ep_n - 1)
    sent(3, arecv, tp_n - 1)
    sent(4, ibox, half)
    sent(10, ibox, half - 1)
    sent(5, mid, 2 * yn - 1)
    sent(6, srecv, tp_n - 1)
    for g in range(2):
        sent((7, 11)[g], xg.at[g], 2 * yn - 1)
        sent((8, 12)[g], erecv.at[g], tp_n - 1)
    sent(9, rrecv, ep_n - 1)


def hand_over(a, b, c, x, y, z, sem):
    copies = [
        pltpu.make_async_copy(src, dst, sem.at[i])
        for i, (src, dst) in enumerate(((a, x), (b, y), (c, z)))
    ]
    for one in copies:
        one.start()
    for one in copies:
        one.wait()


def body(
    ep_n,
    tp_n,
    tokens,
    attn_gain,
    query_weight,
    key_weight,
    value_weight,
    query_gain,
    stick_bias,
    key_cache,
    value_cache,
    lengths,
    out_weight,
    mix_gain,
    route_ids,
    route_weights,
    expert_gate,
    expert_up,
    expert_down,
    side_gate,
    side_up,
    side_down,
    branch_gate,
):
    seqs, width = tokens.shape
    slots = key_cache.shape[2]
    kt = width // 128
    any_ = pl.BlockSpec(memory_space=pl.ANY)
    vmem = pl.BlockSpec(memory_space=pltpu.VMEM)
    specs = [any_] * 21
    specs[6] = pl.BlockSpec(memory_space=pltpu.SMEM)
    V = pltpu.VMEM
    scratch = [
        V((seqs, width), BF16),
        V((1, width), F32),
        V((1, width), F32),
        V((1, DH), F32),
        V((1, width), F32),
        V((2 * query_weight.shape[0], 2 * DH), BF16),
        V((seqs, slots, DH), BF16),
        V((seqs, slots, DH), BF16),
        V(out_weight.shape, BF16),
        V(expert_gate.shape[:0:-1], BF16),
        V(expert_up.shape[:0:-1], BF16),
        V(expert_down.shape[1:], BF16),
        V(side_gate.shape[::-1], BF16),
        V(side_up.shape[::-1], BF16),
        V(side_down.shape, BF16),
        V((slots, slots), BF16),
        V((kt, seqs, 128), F32),
        V((kt, seqs, 128), BF16),
        V((ep_n, seqs, 128), BF16),
        V((ep_n, 2, seqs, 128), BF16),
        V((ep_n, 2, seqs, 128), BF16),
        V((kt, seqs, 128), BF16),
        V((tp_n, seqs, 128), BF16),
        V((kt, seqs, 128), BF16),
        V((seqs, width), BF16),
        V((2 * ep_n, 128), F32),
        V((ep_n, 1, 256), F32),
        V((ep_n, 1, 256), F32),
        V((ep_n, 128), F32),
        V((2, kt, ep_n, 128), BF16),
        V((ep_n, width), BF16),
        V((kt, seqs, 128), BF16),
        V((tp_n, seqs, 128), BF16),
        V((2, tp_n, ep_n // 2, 128), BF16),
        V((2, tp_n, ep_n // 2, 128), BF16),
        V((ep_n, 1, 128), F32),
        V((ep_n, 1, 128), F32),
        V((ep_n, *query_weight.shape), BF16),
        pltpu.SMEM((seqs,), jnp.int32),
        pltpu.SMEM((2, seqs), jnp.int32),
        pltpu.SMEM((2, seqs), F32),
        V((ep_n // 4 - 1, seqs, 128), BF16),
        V((2, seqs, DH), F32),
        V((2, seqs, DH), F32),
        pltpu.SemaphoreType.REGULAR((tp_n // XN // 2 + 1,)),
        pltpu.SemaphoreType.REGULAR((tp_n // XN // 2 + 1,)),
        pltpu.SemaphoreType.REGULAR((2,)),
        pltpu.SemaphoreType.REGULAR((2,)),
        pltpu.SemaphoreType.DMA((20,)),
        pltpu.SemaphoreType.DMA((13,)),
        pltpu.SemaphoreType.DMA((13,)),
        pltpu.SemaphoreType.DMA((3,)),
        pltpu.SemaphoreType.DMA((ep_n + 2,)),
    ]
    shapes = ((seqs, width // tp_n), (seqs, DH), (seqs, DH))
    results = pl.pallas_call(
        functools.partial(kernel, ep_n, tp_n),
        out_shape=tuple(V(s, BF16) for s in shapes),
        in_specs=specs,
        out_specs=(vmem, vmem, vmem),
        scratch_shapes=scratch,
        compiler_params=pltpu.CompilerParams(
            collective_id=0, has_side_effects=True, vmem_limit_bytes=60 * 1024 * 1024
        ),
        name="decode_layer",
    )(
        tokens,
        attn_gain.reshape(1, -1),
        query_weight,
        key_weight,
        value_weight,
        query_gain.reshape(1, -1),
        stick_bias,
        key_cache,
        value_cache,
        lengths,
        out_weight,
        mix_gain.reshape(1, -1),
        route_ids.T,
        route_weights.T,
        jnp.swapaxes(expert_gate, 1, 2),
        jnp.swapaxes(expert_up, 1, 2),
        expert_down,
        side_gate.T,
        side_up.T,
        side_down,
        branch_gate.reshape(1, -1),
    )
    return pl.pallas_call(
        hand_over,
        out_shape=tuple(jax.ShapeDtypeStruct(s, BF16) for s in shapes),
        in_specs=[vmem] * 3,
        out_specs=[any_] * 3,
        scratch_shapes=[pltpu.SemaphoreType.DMA((3,))],
        name="hand_over",
    )(*[pltpu.with_memory_space_constraint(r, pltpu.VMEM) for r in results])


def solution(mesh):
    in_specs = (
        P("ep", None),
        P(),
        P("ep", "tp"),
        P("ep", "tp"),
        P("ep", "tp"),
        P(),
        P("tp"),
        P("ep", "tp", None, None),
        P("ep", "tp", None, None),
        P("ep"),
        P("tp", None),
        P(),
        P("ep", None),
        P("ep", None),
        P("ep", None, "tp"),
        P("ep", None, "tp"),
        P("ep", "tp", None),
        P(None, "tp"),
        P(None, "tp"),
        P("tp", None),
        P(),
    )
    out_specs = (P("ep", "tp"), P("ep", "tp"), P("ep", "tp"))
    step = functools.partial(body, mesh.shape["ep"], mesh.shape["tp"])
    return jax.shard_map(step, mesh=mesh, in_specs=in_specs, out_specs=out_specs, check_vma=False)
```
